32 devices in a mesh: ep: 8 (over z, y), tp: 4 (over x, core).
Axes of the slice: x: 2, y: 2, z: 4, core: 2. Of those that a mesh axis runs over, the one named last changes fastest.
Arguments:
- conv_value: bfloat16 [3072, 2048], P('ep', 'tp'), may hold values from -36 to 36
- conv_gate: bfloat16 [3072, 2048], P('ep', 'tp'), may hold values from -8 to 8
- conv_taps: bfloat16 [31, 2048], P(None, 'tp'), may hold values from -1 to 1
- conv_gain: float32 [2048], P('tp'), may hold values from 0.1 to 1.9
- conv_proj: bfloat16 [2048, 2048], P('tp'), may hold values from -0.125 to 0.125
- moe_tokens: bfloat16 [3072, 2048], P('ep'), may hold values from -6 to 6
- moe_gain: float32 [2048], replicated, may hold values from 0.1 to 1.9
- routes: int32 [3072, 2], P('ep'), may hold values from 0 to 7, all different within a row; in each aligned block of 384 rows (0 to 383, 384 to 767, ...) at most 144 rows name the same one
- route_weights: float32 [3072, 2], P('ep'), may hold values from 0.3 to 3
- expert_gate: bfloat16 [8, 2048, 1024], P('ep', None, 'tp'), may hold values from -0.125 to 0.125
- expert_up: bfloat16 [8, 2048, 1024], P('ep', None, 'tp'), may hold values from -0.125 to 0.125
- expert_down: bfloat16 [8, 1024, 2048], P('ep', 'tp'), may hold values from -0.1875 to 0.1875
- shared_gate: bfloat16 [2048, 256], replicated, may hold values from -0.125 to 0.125
- shared_up: bfloat16 [2048, 256], replicated, may hold values from -0.125 to 0.125
- shared_down: bfloat16 [256, 2048], P(None, 'tp'), may hold values from -0.375 to 0.375
Outputs:
- conv_result: bfloat16 [3072, 2048], P('ep', 'tp')
- moe_result: bfloat16 [3072, 2048], P('ep', 'tp')
The draws below stay inside these ranges and needn't reach their ends.
Inputs may be any that keep to these rules, and one draw needn't show every extreme that they name: `routes`: each row names 2 different experts. Among the 384 rows of one index of ep (aligned blocks in order) no expert is named more than 144 times, and in some blocks one expert is named exactly 144 times.
All inputs are finite; a program needn't handle non-finite values.
Results may differ from the reference program's by a relative error of at most 0.01.
Values may be sent and summed in bfloat16 or wider, within the bound.
A program may use at most 64 MiB of HBM per device.

```python
import math
import jax
import jax.numpy as jnp
import numpy as np
from jax import lax

D = 2048
KERNEL = 31
EXPERT_FF = 1024
SHARED_FF = 256
TOPK = 2
TOK_DEV = 384
TOKENS = 3072
EXPERTS = 8
CAPACITY = 144
N_EP = 8
N_TP = 4


def draw_conv_value(key, part):
    first, second = jax.random.split(jax.random.fold_in(key, 11))
    position = jnp.arange(D, dtype=jnp.float32) / (D - 1)
    rough = jnp.exp(jax.random.uniform(second, (D,), jnp.float32, -0.35, 0.35))
    column_scale = jnp.exp(jnp.log(0.5) + position * jnp.log(8.0)) * rough
    values = jnp.clip(jax.random.normal(first, (TOKENS, D), jnp.float32), -6.0, 6.0)
    return (values * column_scale[None, :]).astype(jnp.bfloat16)


def levels(own_key, extent, pieces, low, largest):
    level, own = 1.0, jax.random.fold_in(own_key, 6)
    for dim, blocks in pieces:
        draws = jnp.exp(jax.random.uniform(jax.random.fold_in(own, dim), (blocks,), jnp.float32, low / len(pieces), largest / len(pieces)))
        level = level * jnp.repeat(draws, extent[dim] // blocks).reshape([-1 if axis == dim else 1 for axis in range(len(extent))])
    return level


def shared_out(key, own, number, rows, amount, top, most, lean):
    ranking = jax.random.permutation(key, amount)
    packed, ordinary = portions_of(amount, rows * top, most, lean, True), portions_of(amount, rows * top, most, lean, False)
    places = jnp.arange(amount)

    def named(lengths, turn):
        used = int((lengths > 0).sum())
        fixed = max(1, used // 4)
        shifted = fixed + (places - fixed + turn * (used - fixed)) % max(1, amount - fixed)
        return jnp.zeros((amount,), jnp.int32).at[ranking[jnp.where(places < fixed, places, shifted)]].set(jnp.asarray(lengths, jnp.int32))

    lengths = jnp.where(number % 4 == 0, named(packed, number // 4), named(ordinary, number - number // 4 - 1))
    mixed = jax.random.permutation(jax.random.fold_in(own, 3), amount)
    donor, taker = mixed[0:amount // 2 * 2:2], mixed[1:amount // 2 * 2:2]
    room = jnp.minimum(lengths[donor] - 1, most - lengths[taker]) // 2
    room = jnp.where((donor == ranking[0]) | (taker == ranking[0]) | (lengths[taker] == 0), 0, jnp.maximum(room, 0))
    shifted = jax.random.randint(jax.random.fold_in(own, 4), (amount // 2,), 0, 1 << 20) % (room + 1)
    lengths = lengths.at[donor].add(-shifted).at[taker].add(shifted)
    members = jnp.searchsorted(jnp.cumsum(lengths), jnp.arange(rows * top), side="right").astype(jnp.int32)
    table = members.reshape(top, rows).T
    table = table[jax.random.permutation(jax.random.fold_in(own, 1), rows)]
    turn = jax.random.randint(jax.random.fold_in(own, 2), (rows, 1), 0, top)
    return jnp.take_along_axis(table, (jnp.arange(top)[None, :] + turn) % top, axis=1)


def portions_of(amount, total, reach, skew, full):
    portions = [(1 << 20) // math.isqrt(grade ** skew) + 1 for grade in range(1, amount + 1)]
    largest = reach if full else min(reach, max(-(-total // amount), total * portions[0] // sum(portions)))
    least = 1 if total - largest >= amount - 1 else 0
    given, spare = [largest] + [least] * (amount - 1), total - largest - least * (amount - 1)
    while spare > 0:
        movable = [i for i in range(1, amount) if given[i] < largest] or [i for i in range(1, amount) if given[i] < reach]
        mass, budget = sum([portions[i] for i in movable]), spare
        for i in movable:
            extra = min(reach - given[i], max(1, budget * portions[i] // mass), spare)
            given[i] = given[i] + extra
            spare = spare - extra
    return np.array(given)


def normal_values(stream_key, dims, deviation, limit, shards=(), kind=jnp.bfloat16):
    values = jax.random.normal(stream_key, dims, jnp.float32) * deviation
    if len(shards) > 0:
        values = levels(stream_key, dims, shards, -0.22, 0.18) * values
    return jnp.clip(values, min=-limit, max=limit).astype(kind)


def setup_inputs(seed: int = 0) -> dict:
    streams_of = jax.random.split(jax.random.key(seed), 16)
    conv_value = draw_conv_value(jax.random.fold_in(streams_of[15], 71), 0)
    conv_gate = normal_values(streams_of[1], (TOKENS, D), 1.5, 8.0, ((0, 8), (1, 4)))
    conv_taps = normal_values(streams_of[2], (KERNEL, D), KERNEL ** -0.5, 1.0, ((1, 4),))
    conv_gain = jnp.clip(1.0 + 0.18 * jax.random.normal(streams_of[3], (D,), jnp.float32), 0.1, 1.9)
    conv_proj = normal_values(streams_of[4], (D, D), D ** -0.5, 0.125, ((0, 4),))
    moe_tokens = normal_values(streams_of[5], (TOKENS, D), 1.0, 6.0, ((0, 8),))
    moe_gain = jnp.clip(1.0 + 0.18 * jax.random.normal(streams_of[6], (D,), jnp.float32), 0.1, 1.9)
    routes_keys = jax.random.split(jax.random.fold_in(streams_of[7], 1), TOKENS // TOK_DEV)
    routes_turns = jax.random.permutation(jax.random.fold_in(streams_of[7], 3), TOKENS // TOK_DEV)
    routes = jax.vmap(lambda own, number: shared_out(jax.random.fold_in(streams_of[7], 2), own, number, TOK_DEV, EXPERTS, TOPK, CAPACITY, 1))(routes_keys, routes_turns).reshape((TOKENS, TOPK))
    route_weights = jnp.clip(jnp.exp(math.log(3.0) - 2.3025851 * jax.random.uniform(streams_of[8], (TOKENS, TOPK), jnp.float32) ** levels(streams_of[8], (TOKENS, TOPK), ((0, 8),), -0.2, 0.2)), 0.3, 3.0)
    expert_gate = normal_values(streams_of[9], (EXPERTS, D, EXPERT_FF), D ** -0.5, 0.125, ((0, 8), (2, 4)))
    expert_up = normal_values(streams_of[10], (EXPERTS, D, EXPERT_FF), D ** -0.5, 0.125, ((0, 8), (2, 4)))
    expert_down = normal_values(streams_of[11], (EXPERTS, EXPERT_FF, D), EXPERT_FF ** -0.5, 0.1875, ((0, 8), (1, 4)))
    shared_gate = normal_values(streams_of[12], (D, SHARED_FF), D ** -0.5, 0.125)
    shared_up = normal_values(streams_of[13], (D, SHARED_FF), D ** -0.5, 0.125)
    shared_down = normal_values(streams_of[14], (SHARED_FF, D), SHARED_FF ** -0.5, 0.375, ((1, 4),))
    return {"conv_value": conv_value, "conv_gate": conv_gate, "conv_taps": conv_taps, "conv_gain": conv_gain, "conv_proj": conv_proj, "moe_tokens": moe_tokens, "moe_gain": moe_gain, "routes": routes, "route_weights": route_weights, "expert_gate": expert_gate, "expert_up": expert_up, "expert_down": expert_down, "shared_gate": shared_gate, "shared_up": shared_up, "shared_down": shared_down}


epsilon = 1e-05

def rounded_block(product):
    return lax.optimization_barrier(product.astype(jnp.bfloat16)).astype(jnp.float32)

def reference(conv_value, conv_gate, conv_taps, conv_gain, conv_proj, moe_tokens, moe_gain, routes, route_weights, expert_gate, expert_up, expert_down, shared_gate, shared_up, shared_down):
    gated_rows = (conv_value.astype(jnp.float32) * jax.nn.sigmoid(conv_gate.astype(jnp.float32))).astype(jnp.bfloat16)
    padded = jnp.concatenate([jnp.zeros((KERNEL - 1, D), jnp.bfloat16), gated_rows], axis=0).astype(jnp.float32)
    tap_weights = conv_taps.astype(jnp.float32)
    convolved = jnp.zeros((TOKENS, D), jnp.float32)
    for offset in range(KERNEL):
        convolved = convolved + tap_weights[offset][None, :] * padded[offset:offset + TOKENS]
    average = lax.optimization_barrier(jnp.sum(convolved, axis=1)) / D
    variance = lax.optimization_barrier(jnp.sum(convolved * convolved, axis=1)) / D - average * average
    scaled = (convolved - average[:, None]) * lax.rsqrt(variance + epsilon)[:, None] * conv_gain[None, :]
    activated = jax.nn.silu(scaled).astype(jnp.bfloat16)
    block_width = D // N_TP
    conv_total = jnp.zeros((TOKENS, D), jnp.float32)
    for block in range(N_TP):
        product = jnp.dot(activated[:, block * block_width:(block + 1) * block_width], conv_proj[block * block_width:(block + 1) * block_width], preferred_element_type=jnp.float32)
        conv_total = conv_total + rounded_block(product)
    conv_result = conv_total.astype(jnp.bfloat16)
    tokens = moe_tokens.astype(jnp.float32)
    token_mean = lax.optimization_barrier(jnp.mean(tokens, axis=1, keepdims=True))
    centered = tokens - token_mean
    token_var = lax.optimization_barrier(jnp.mean(centered * centered, axis=1, keepdims=True))
    normalized = (centered * lax.rsqrt(token_var + epsilon) * moe_gain[None, :]).astype(jnp.bfloat16)
    shared_hidden = (jax.nn.silu(jnp.dot(normalized, shared_gate, preferred_element_type=jnp.float32)) * jnp.dot(normalized, shared_up, preferred_element_type=jnp.float32)).astype(jnp.bfloat16)
    shared_part = jnp.dot(shared_hidden, shared_down, preferred_element_type=jnp.float32)
    entries = TOKENS * TOPK
    flat_routes = routes.reshape(-1).astype(jnp.int32)
    flat_index = jnp.arange(entries, dtype=jnp.int32)
    slot_count = N_EP * CAPACITY
    hidden_width = EXPERT_FF // N_TP

    def one_expert(carried, expert):
        chosen = (flat_routes == expert).astype(jnp.int32)
        order = (jnp.cumsum(chosen) - chosen).astype(jnp.int32)
        target = jnp.where(chosen > 0, order, slot_count).astype(jnp.int32)
        source_row = jnp.zeros((slot_count,), jnp.int32).at[target].set(flat_index, mode='drop')
        filled = jnp.zeros((slot_count,), jnp.int32).at[target].set(jnp.ones((entries,), jnp.int32), mode='drop')
        rows_in = normalized[(source_row // TOPK).astype(jnp.int32)]
        hidden = (jax.nn.silu(jnp.dot(rows_in, expert_gate[expert], preferred_element_type=jnp.float32)) * jnp.dot(rows_in, expert_up[expert], preferred_element_type=jnp.float32)).astype(jnp.bfloat16)
        down_rows = expert_down[expert]
        total = jnp.zeros((slot_count, D), jnp.float32)
        for block in range(N_TP):
            product = jnp.dot(hidden[:, block * hidden_width:(block + 1) * hidden_width], down_rows[block * hidden_width:(block + 1) * hidden_width], preferred_element_type=jnp.float32)
            total = total + rounded_block(product)
        write_at = jnp.where(filled > 0, source_row, entries).astype(jnp.int32)
        carried = carried.at[write_at].set(total.astype(jnp.bfloat16), mode='drop')
        return (carried, None)
    expert_rows, _ = lax.scan(one_expert, jnp.zeros((entries, D), jnp.bfloat16), jnp.arange(EXPERTS, dtype=jnp.int32))
    expert_rows = expert_rows.reshape(TOKENS, TOPK, D)
    moe_total = shared_part
    for choice_index in range(TOPK):
        moe_total = moe_total + route_weights[:, choice_index][:, None] * expert_rows[:, choice_index].astype(jnp.float32)
    moe_result = moe_total.astype(jnp.bfloat16)
    return (conv_result, moe_result)
```

```python
import functools

import jax
import jax.numpy as jnp
from jax import lax
from jax.experimental import pallas as pl
from jax.experimental.pallas import tpu as pltpu
from jax.sharding import PartitionSpec as P

epsilon = 1e-05
MESH = pl.DeviceIdType.MESH
f32 = jnp.float32
bf16 = jnp.bfloat16


def dot(a, b):
    return jnp.dot(a, b, preferred_element_type=f32)


def kernel(
    n, tp, cap,
    tok, gain, routes_t, weights_t, act,
    gate_h, up_h, down_h, sg_h, su_h, sd_h, proj_h,
    conv_out, moe_out,
    gate, up, down, sg, su, sd, proj,
    norm, rank_s, wt_s, out_buf, arr, p_send, p_own, p_recv, q_send, q_recv, fin, ret,
    shared, c_send, c_own, c_recv, cq_send, cq_recv,
    load_sem, a2a_s, a2a_r, fc_s, fc_r, fx_s, fx_r, f2_s, f2_r,
    p_s, p_r, q_s, q_r, ret_s, ret_r, c_sem,
):
    i = lax.axis_index("ep")
    j = lax.axis_index("tp")
    jx, jc = lax.div(j, 2), lax.rem(j, 2)
    partner = jx * 2 + 1 - jc
    across = (1 - jx) * 2 + jc
    rows, width = tok.shape
    quarter = width // tp

    barrier = pltpu.get_barrier_semaphore()

    def greet(d, _):
        pl.semaphore_signal(
            barrier, inc=1, device_id=(lax.rem(i + d, n), j), device_id_type=MESH
        )
        return 0

    lax.fori_loop(1, n, greet, 0)
    for t in (partner, across):
        pl.semaphore_signal(barrier, inc=1, device_id=(i, t), device_id_type=MESH)

    loads = [
        pltpu.make_async_copy(src, dst, load_sem.at[k])
        for k, (src, dst) in enumerate(
            ((proj_h, proj), (gate_h.at[0], gate), (up_h.at[0], up), (down_h.at[0], down),
             (sg_h, sg), (su_h, su), (sd_h, sd))
        )
    ]
    for load in loads:
        load.start()

    def columns(block):
        return pl.ds(pl.multiple_of(block * quarter, quarter), quarter)

    experts = rank_s.shape[0]
    e_iota = lax.broadcasted_iota(jnp.int32, (experts, rows), 0)
    chosen = jnp.zeros((experts, rows), f32)
    weight = jnp.zeros((experts, rows), f32)
    for k in range(routes_t.shape[0]):
        hit = routes_t[k : k + 1, :] == e_iota
        chosen = jnp.where(hit, 1.0, chosen)
        weight = jnp.where(hit, weights_t[k : k + 1, :], weight)
    earlier = (
        lax.broadcasted_iota(jnp.int32, (rows, rows), 0)
        < lax.broadcasted_iota(jnp.int32, (rows, rows), 1)
    )
    rank = dot(chosen.astype(bf16), jnp.where(earlier, 1.0, 0.0).astype(bf16))
    rank_s[...] = jnp.where(chosen > 0.0, rank, -1.0).astype(jnp.int32)
    wt_s[...] = weight

    piece = rows // 8

    def norm_rows(r, _):
        at = pl.ds(pl.multiple_of(r * piece, piece), piece)
        x = tok[at, :].astype(f32)
        c = x - jnp.mean(x, axis=1, keepdims=True)
        v = jnp.mean(c * c, axis=1, keepdims=True)
        norm[at, :] = (c * lax.rsqrt(v + epsilon) * gain[...]).astype(bf16)
        return 0

    lax.fori_loop(0, 8, norm_rows, 0)

    slot = lax.broadcasted_iota(jnp.int32, (cap, rows), 0)

    def pick(e):
        return slot == rank_s[pl.ds(e, 1), :]

    def fill(d, _):
        e = lax.rem(i + d, n)
        chosen_rows = jnp.where(pick(e), 1.0, 0.0).astype(bf16)
        out_buf[e] = dot(chosen_rows, norm[:, columns(j)]).astype(bf16)
        return 0

    lax.fori_loop(1, n, fill, 0)
    pl.semaphore_wait(barrier, n + 1)

    def to_expert(e):
        return pltpu.make_async_remote_copy(
            src_ref=out_buf.at[e], dst_ref=arr.at[j, i], send_sem=a2a_s.at[e],
            recv_sem=a2a_r.at[i], device_id=(e, j), device_id_type=MESH,
        )

    def from_source(s):
        return pltpu.make_async_remote_copy(
            src_ref=out_buf.at[s], dst_ref=arr.at[j, s], send_sem=a2a_s.at[s],
            recv_sem=a2a_r.at[s], device_id=(s, j), device_id_type=MESH,
        )

    def send(d, _):
        to_expert(lax.rem(i + d, n)).start()
        return 0

    lax.fori_loop(1, n, send, 0)

    def forward(block, s, to, ss, rs):
        return pltpu.make_async_remote_copy(
            src_ref=arr.at[block, s], dst_ref=arr.at[block, s], send_sem=ss.at[s],
            recv_sem=rs.at[s], device_id=(i, to), device_id_type=MESH,
        )

    def move(src, dst, ss, rs, ep_at, tp_at):
        return pltpu.make_async_remote_copy(
            src_ref=src, dst_ref=dst, send_sem=ss, recv_sem=rs,
            device_id=(ep_at, tp_at), device_id_type=MESH,
        )

    loads[0].wait()
    for half in range(2):
        c_send[half] = dot(act[...], proj[:, columns(half * 2 + 1 - jc)]).astype(bf16)
    c_one = move(c_send, c_recv, c_sem.at[0], c_sem.at[1], i, partner)
    c_one.start()
    for half in range(2):
        c_own[half] = dot(act[...], proj[:, columns(half * 2 + jc)]).astype(bf16)
    own_rows = jnp.where(pick(i), 1.0, 0.0).astype(bf16)
    for block in range(tp):
        arr[block, i] = dot(
            own_rows, norm[:, block * quarter : (block + 1) * quarter]
        ).astype(bf16)
    c_one.wait()
    cq_send[...] = (c_own[1 - jx].astype(f32) + c_recv[1 - jx].astype(f32)).astype(bf16)
    c_two = move(cq_send, cq_recv, c_sem.at[2], c_sem.at[3], i, across)
    c_two.start()

    for load in loads[4:]:
        load.wait()
    shared_hidden = (
        jax.nn.silu(dot(norm[...], sg[...])) * dot(norm[...], su[...])
    ).astype(bf16)
    shared[...] = dot(shared_hidden, sd[...])
    for load in loads[1:4]:
        load.wait()

    def p_copy(s):
        return move(p_send.at[s], p_recv.at[s], p_s.at[s], p_r.at[s], i, partner)

    def q_copy(s):
        return move(q_send.at[s], q_recv.at[s], q_s.at[s], q_r.at[s], i, across)

    def back_to(s):
        return move(fin.at[s], ret.at[i], ret_s.at[s], ret_r.at[i], s, j)

    def back_from(e):
        return move(fin.at[e], ret.at[e], ret_s.at[e], ret_r.at[e], e, j)

    block_x = across
    block_2 = (1 - jx) * 2 + 1 - jc

    def step(d, _):
        s0 = lax.rem(i - d + 2 * n, n)
        s1 = lax.rem(i - d + 1 + 2 * n, n)
        s2 = lax.rem(i - d + 2 + 2 * n, n)
        s3 = lax.rem(i - d + 3 + 2 * n, n)
        s4 = lax.rem(i - d + 4 + 2 * n, n)

        @pl.when(d < n)
        def _():
            from_source(s0).wait_recv()
            forward(j, s0, across, fx_s, fx_r).start()
            forward(j, s0, partner, fc_s, fc_r).start()

        @pl.when((d >= 2) & (d - 1 < n))
        def _():
            forward(block_x, s1, across, fx_s, fx_r).wait_recv()
            forward(block_x, s1, partner, f2_s, f2_r).start()

        @pl.when((d >= 3) & (d - 2 < n))
        def _():
            forward(partner, s2, partner, fc_s, fc_r).wait_recv()
            forward(block_2, s2, partner, f2_s, f2_r).wait_recv()

        @pl.when((d >= 2) & (d - 2 < n))
        def _():
            g = jnp.zeros((cap, gate.shape[1]), f32)
            u = jnp.zeros((cap, gate.shape[1]), f32)
            for block in range(tp):
                x = arr[block, s2]
                at = slice(block * quarter, (block + 1) * quarter)
                g = g + dot(x, gate[at, :])
                u = u + dot(x, up[at, :])
            hidden = (jax.nn.silu(g) * u).astype(bf16)
            for half in range(2):
                p_send[s2, half] = dot(hidden, down[:, columns(half * 2 + 1 - jc)]).astype(bf16)
            for half in range(2):
                p_own[s2, half] = dot(hidden, down[:, columns(half * 2 + jc)]).astype(bf16)
            p_copy(s2).start()

        @pl.when((d >= 3) & (d - 3 < n))
        def _():
            p_copy(s3).wait_recv()
            q_send[s3] = (
                p_own[s3, 1 - jx].astype(f32) + p_recv[s3, 1 - jx].astype(f32)
            ).astype(bf16)
            q_copy(s3).start()

        @pl.when((d >= 4) & (d - 4 < n))
        def _():
            q_copy(s4).wait_recv()
            total = (
                p_own[s4, jx].astype(f32) + p_recv[s4, jx].astype(f32) + q_recv[s4].astype(f32)
            ).astype(bf16)

            @pl.when(d == 4)
            def _():
                ret[i] = total

            @pl.when(d > 4)
            def _():
                fin[s4] = total
                back_to(s4).start()

        return 0

    lax.fori_loop(1, n + 4, step, 0)

    c_two.wait()
    conv_out[...] = (
        c_own[jx].astype(f32) + c_recv[jx].astype(f32) + cq_recv[...].astype(f32)
    ).astype(bf16)

    def combine(e):
        hit = pick(e)
        w = wt_s[pl.ds(e, 1), :]
        high = w.astype(bf16).astype(f32)
        low = w - high
        rows_back = ret[e]
        total = jnp.zeros(shared.shape, f32)
        for part in (high, low):
            m = jnp.where(hit, part, 0.0).astype(bf16)
            total = total + lax.dot_general(
                m, rows_back, (((0,), (0,)), ((), ())), preferred_element_type=f32
            )
        shared[...] += total

    combine(i)

    def gather(d, _):
        e = lax.rem(i + d, n)
        back_from(e).wait_recv()
        combine(e)
        return 0

    lax.fori_loop(1, n, gather, 0)
    moe_out[...] = shared[...].astype(bf16)

    def drain(d, _):
        s = lax.rem(i + d, n)
        to_expert(s).wait_send()
        forward(j, s, across, fx_s, fx_r).wait_send()
        forward(j, s, partner, fc_s, fc_r).wait_send()
        forward(block_x, s, partner, f2_s, f2_r).wait_send()
        back_to(s).wait_send()
        return 0

    lax.fori_loop(1, n, drain, 0)

    def drain_all(s, _):
        p_copy(s).wait_send()
        q_copy(s).wait_send()
        return 0

    lax.fori_loop(0, n, drain_all, 0)


def conv_rows(conv_value, conv_gate, conv_taps, conv_gain, model_width):
    tok_rows = conv_value.shape[0]
    taps = conv_taps.shape[0]
    gated_rows = (
        conv_value.astype(f32) * jax.nn.sigmoid(conv_gate.astype(f32))
    ).astype(bf16)
    devices = lax.axis_size("ep")
    previous = lax.ppermute(
        gated_rows[tok_rows - (taps - 1) :], "ep", [(i, i + 1) for i in range(devices - 1)]
    )
    padded = jnp.concatenate([previous, gated_rows], axis=0).astype(f32)
    tap_weights = conv_taps.astype(f32)
    convolved = jnp.zeros(gated_rows.shape, f32)
    for offset in range(taps):
        convolved = convolved + tap_weights[offset][None, :] * padded[offset : offset + tok_rows]
    total_sum, square_sum = lax.psum(
        (jnp.sum(convolved, axis=1), jnp.sum(convolved * convolved, axis=1)), "tp"
    )
    average = total_sum / model_width
    variance = square_sum / model_width - average * average
    scaled = (
        (convolved - average[:, None]) * lax.rsqrt(variance + epsilon)[:, None] * conv_gain[None, :]
    )
    return jax.nn.silu(scaled).astype(bf16)


def local(
    conv_value, conv_gate, conv_taps, conv_gain, conv_proj, moe_tokens, moe_gain, routes,
    route_weights, expert_gate, expert_up, expert_down, shared_gate, shared_up, shared_down,
):
    n, tp = lax.axis_size("ep"), lax.axis_size("tp")
    assert tp == 4
    rows, width = moe_tokens.shape
    quarter = width // tp
    cap = 3 * rows * routes.shape[1] // (2 * n)
    cap = -(-cap // 16) * 16
    ff = expert_gate.shape[2]
    activated = conv_rows(conv_value, conv_gate, conv_taps, conv_gain, width)
    vmem = pl.BlockSpec(memory_space=pltpu.VMEM)
    anywhere = pl.BlockSpec(memory_space=pl.ANY)
    V = pltpu.VMEM
    dma = pltpu.SemaphoreType.DMA
    return pl.pallas_call(
        functools.partial(kernel, n, tp, cap),
        out_shape=(
            jax.ShapeDtypeStruct((rows, quarter), bf16),
            jax.ShapeDtypeStruct((rows, quarter), bf16),
        ),
        in_specs=[vmem] * 5 + [anywhere] * 7,
        out_specs=(vmem, vmem),
        scratch_shapes=[
            V((width, ff), bf16), V((width, ff), bf16), V((ff, width), bf16),
            V(shared_gate.shape, bf16), V(shared_up.shape, bf16), V(shared_down.shape, bf16),
            V(conv_proj.shape, bf16),
            V((rows, width), bf16), V((n, rows), jnp.int32), V((n, rows), f32),
            V((n, cap, quarter), bf16), V((tp, n, cap, quarter), bf16),
            V((n, 2, cap, quarter), bf16), V((n, 2, cap, quarter), bf16),
            V((n, 2, cap, quarter), bf16),
            V((n, cap, quarter), bf16), V((n, cap, quarter), bf16),
            V((n, cap, quarter), bf16), V((n, cap, quarter), bf16),
            V((rows, quarter), f32),
            V((2, rows, quarter), bf16), V((2, rows, quarter), bf16), V((2, rows, quarter), bf16),
            V((rows, quarter), bf16), V((rows, quarter), bf16),
            dma((7,)),
        ] + [dma((n,))] * 14 + [dma((4,))],
        compiler_params=pltpu.CompilerParams(
            collective_id=0, has_side_effects=True, vmem_limit_bytes=60 * 1024 * 1024
        ),
    )(
        moe_tokens, moe_gain[None, :], routes.T, route_weights.T, activated,
        expert_gate, expert_up, expert_down, shared_gate, shared_up, shared_down, conv_proj,
    )


def solution(mesh):
    placed = (
        P("ep", "tp"),
        P("ep", "tp"),
        P(None, "tp"),
        P("tp"),
        P("tp", None),
        P("ep", None),
        P(),
        P("ep", None),
        P("ep", None),
        P("ep", None, "tp"),
        P("ep", None, "tp"),
        P("ep", "tp", None),
        P(),
        P(),
        P(None, "tp"),
    )
    return jax.shard_map(
        local, mesh=mesh, in_specs=placed, out_specs=(P("ep", "tp"), P("ep", "tp")), check_vma=False
    )
```

```python
import functools

import jax
import jax.numpy as jnp
from jax import lax
from jax.experimental import pallas as pl
from jax.experimental.pallas import tpu as pltpu
from jax.sharding import PartitionSpec as P

epsilon = 1e-05
MESH = pl.DeviceIdType.MESH
f32 = jnp.float32
bf16 = jnp.bfloat16


def dot(a, b):
    return jnp.dot(a, b, preferred_element_type=f32)


def kernel(
    n, tp, cap,
    tok, gain, routes_t, weights_t, conv_gain, value_h, cgate_h, taps_h,
    gate_h, up_h, down_h, sg_h, su_h, sd_h, proj_h,
    conv_out, moe_out,
    gate, up, down, sg, su, sd, proj,
    norm, rank_s, wt_s, out_buf, arr, p_send, p_own, p_recv, q_send, q_recv, fin, ret,
    value, cgate, taps, pad, halo_out, halo_in, conv, stats, stat_a, stat_b, stat_c, stat_d,
    shared, c_send, c_own, c_recv, cq_send, cq_recv,
    load_sem, a2a_s, a2a_r, fc_s, fc_r, fx_s, fx_r, f2_s, f2_r,
    p_s, p_r, q_s, q_r, ret_s, ret_r, c_sem, h_sem,
):
    i = lax.axis_index("ep")
    j = lax.axis_index("tp")
    jx, jc = lax.div(j, 2), lax.rem(j, 2)
    partner = jx * 2 + 1 - jc
    across = (1 - jx) * 2 + jc
    rows, width = tok.shape
    quarter = width // tp

    barrier = pltpu.get_barrier_semaphore()

    def greet(d, _):
        pl.semaphore_signal(
            barrier, inc=1, device_id=(lax.rem(i + d, n), j), device_id_type=MESH
        )
        return 0

    lax.fori_loop(1, n, greet, 0)
    for t in (partner, across):
        pl.semaphore_signal(barrier, inc=1, device_id=(i, t), device_id_type=MESH)

    loads = [
        pltpu.make_async_copy(src, dst, load_sem.at[k])
        for k, (src, dst) in enumerate(
            ((proj_h, proj), (gate_h.at[0], gate), (up_h.at[0], up), (down_h.at[0], down),
             (sg_h, sg), (su_h, su), (sd_h, sd), (value_h, value), (cgate_h, cgate),
             (taps_h, taps))
        )
    ]
    for load in loads:
        load.start()

    def columns(block):
        return pl.ds(pl.multiple_of(block * quarter, quarter), quarter)

    experts = rank_s.shape[0]
    e_iota = lax.broadcasted_iota(jnp.int32, (experts, rows), 0)
    chosen = jnp.zeros((experts, rows), f32)
    weight = jnp.zeros((experts, rows), f32)
    for k in range(routes_t.shape[0]):
        hit = routes_t[k : k + 1, :] == e_iota
        chosen = jnp.where(hit, 1.0, chosen)
        weight = jnp.where(hit, weights_t[k : k + 1, :], weight)
    earlier = (
        lax.broadcasted_iota(jnp.int32, (rows, rows), 0)
        < lax.broadcasted_iota(jnp.int32, (rows, rows), 1)
    )
    rank = dot(chosen.astype(bf16), jnp.where(earlier, 1.0, 0.0).astype(bf16))
    rank_s[...] = jnp.where(chosen > 0.0, rank, -1.0).astype(jnp.int32)
    wt_s[...] = weight

    piece = rows // 8

    def norm_rows(r, _):
        at = pl.ds(pl.multiple_of(r * piece, piece), piece)
        x = tok[at, :].astype(f32)
        c = x - jnp.mean(x, axis=1, keepdims=True)
        v = jnp.mean(c * c, axis=1, keepdims=True)
        norm[at, :] = (c * lax.rsqrt(v + epsilon) * gain[...]).astype(bf16)
        return 0

    lax.fori_loop(0, 8, norm_rows, 0)

    slot = lax.broadcasted_iota(jnp.int32, (cap, rows), 0)

    def pick(e):
        return slot == rank_s[pl.ds(e, 1), :]

    def fill(d, _):
        e = lax.rem(i + d, n)
        chosen_rows = jnp.where(pick(e), 1.0, 0.0).astype(bf16)
        out_buf[e] = dot(chosen_rows, norm[:, columns(j)]).astype(bf16)
        return 0

    lax.fori_loop(1, n, fill, 0)

    for load in loads[7:]:
        load.wait()
    lead = halo_out.shape[0]
    gated = (value[...].astype(f32) * jax.nn.sigmoid(cgate[...].astype(f32))).astype(bf16)
    pad[lead:, :] = gated.astype(f32)
    halo_out[...] = gated[rows - lead :, :]
    pl.semaphore_wait(barrier, n + 1)

    def halo(ep_at):
        return pltpu.make_async_remote_copy(
            src_ref=halo_out, dst_ref=halo_in, send_sem=h_sem.at[0], recv_sem=h_sem.at[1],
            device_id=(ep_at, j), device_id_type=MESH,
        )

    @pl.when(i < n - 1)
    def _():
        halo(i + 1).start()

    def to_expert(e):
        return pltpu.make_async_remote_copy(
            src_ref=out_buf.at[e], dst_ref=arr.at[j, i], send_sem=a2a_s.at[e],
            recv_sem=a2a_r.at[i], device_id=(e, j), device_id_type=MESH,
        )

    def from_source(s):
        return pltpu.make_async_remote_copy(
            src_ref=out_buf.at[s], dst_ref=arr.at[j, s], send_sem=a2a_s.at[s],
            recv_sem=a2a_r.at[s], device_id=(s, j), device_id_type=MESH,
        )

    def send(d, _):
        to_expert(lax.rem(i + d, n)).start()
        return 0

    lax.fori_loop(1, n, send, 0)

    def forward(block, s, to, ss, rs):
        return pltpu.make_async_remote_copy(
            src_ref=arr.at[block, s], dst_ref=arr.at[block, s], send_sem=ss.at[s],
            recv_sem=rs.at[s], device_id=(i, to), device_id_type=MESH,
        )

    def move(src, dst, ss, rs, ep_at, tp_at):
        return pltpu.make_async_remote_copy(
            src_ref=src, dst_ref=dst, send_sem=ss, recv_sem=rs,
            device_id=(ep_at, tp_at), device_id_type=MESH,
        )

    own_rows = jnp.where(pick(i), 1.0, 0.0).astype(bf16)
    for block in range(tp):
        arr[block, i] = dot(
            own_rows, norm[:, block * quarter : (block + 1) * quarter]
        ).astype(bf16)
    for load in loads[:7]:
        load.wait()

    @pl.when(i == 0)
    def _():
        pad[:lead, :] = jnp.zeros((lead, quarter), f32)

    @pl.when(i > 0)
    def _():
        halo(i - 1).wait_recv()
        pad[:lead, :] = halo_in[...].astype(f32)

    taken = rows // 4
    lanes = 128

    def conv_piece(q):
        first = pl.multiple_of(q * taken, taken)
        weights = taps[...].astype(f32)
        skip = lead - (taps.shape[0] - 1)
        sums = jnp.zeros((taken, 1), f32)
        squares = jnp.zeros((taken, 1), f32)
        for c in range(quarter // lanes):
            at = slice(c * lanes, (c + 1) * lanes)
            window = pad[pl.ds(first, taken + lead), at]
            total = jnp.zeros((taken, lanes), f32)
            for low in range(8):
                turned = window if low == 0 else pltpu.roll(window, taken + lead - low, 0)
                for tap in range(taps.shape[0]):
                    if (skip + tap) % 8 == low:
                        begin = skip + tap - low
                        total = total + weights[tap : tap + 1, at] * turned[begin : begin + taken]
            conv[pl.ds(first, taken), at] = total
            sums = sums + jnp.sum(total, axis=1, keepdims=True)
            squares = squares + jnp.sum(total * total, axis=1, keepdims=True)
        lane = lax.broadcasted_iota(jnp.int32, (taken, lanes), 1)
        stats[pl.ds(first, taken), :] = jnp.where(lane == 0, sums, squares)

    def stat_one():
        return move(stat_a, stat_b, c_sem.at[4], c_sem.at[5], i, partner)

    def stat_two():
        return move(stat_c, stat_d, c_sem.at[6], c_sem.at[7], i, across)

    def c_one():
        return move(c_send, c_recv, c_sem.at[0], c_sem.at[1], i, partner)

    def c_two():
        return move(cq_send, cq_recv, c_sem.at[2], c_sem.at[3], i, across)

    def conv_product():
        both = stat_c[...] + stat_d[...]
        spread = jnp.concatenate([both] * (lanes // 8), axis=0).T
        average = spread[:, 0:1] / width
        variance = spread[:, 1:2] / width - average * average
        scaled = (conv[...] - average) * lax.rsqrt(variance + epsilon) * conv_gain[...]
        act = jax.nn.silu(scaled).astype(bf16)
        for half in range(2):
            c_send[half] = dot(act, proj[:, columns(half * 2 + 1 - jc)]).astype(bf16)
        for half in range(2):
            c_own[half] = dot(act, proj[:, columns(half * 2 + jc)]).astype(bf16)

    def p_copy(s):
        return move(p_send.at[s], p_recv.at[s], p_s.at[s], p_r.at[s], i, partner)

    def q_copy(s):
        return move(q_send.at[s], q_recv.at[s], q_s.at[s], q_r.at[s], i, across)

    def back_to(s):
        return move(fin.at[s], ret.at[i], ret_s.at[s], ret_r.at[i], s, j)

    def back_from(e):
        return move(fin.at[e], ret.at[e], ret_s.at[e], ret_r.at[e], e, j)

    block_x = across
    block_2 = (1 - jx) * 2 + 1 - jc

    def step(d, _):
        s0 = lax.rem(i - d + 2 * n, n)
        s1 = lax.rem(i - d + 1 + 2 * n, n)
        s2 = lax.rem(i - d + 2 + 2 * n, n)
        s3 = lax.rem(i - d + 3 + 2 * n, n)
        s4 = lax.rem(i - d + 4 + 2 * n, n)

        @pl.when(d < n)
        def _():
            from_source(s0).wait_recv()
            forward(j, s0, across, fx_s, fx_r).start()
            forward(j, s0, partner, fc_s, fc_r).start()

        @pl.when((d >= 2) & (d - 1 < n))
        def _():
            forward(block_x, s1, across, fx_s, fx_r).wait_recv()
            forward(block_x, s1, partner, f2_s, f2_r).start()

        @pl.when((d >= 3) & (d - 2 < n))
        def _():
            forward(partner, s2, partner, fc_s, fc_r).wait_recv()
            forward(block_2, s2, partner, f2_s, f2_r).wait_recv()

        @pl.when((d >= 2) & (d - 2 < n))
        def _():
            g = jnp.zeros((cap, gate.shape[1]), f32)
            u = jnp.zeros((cap, gate.shape[1]), f32)
            for block in range(tp):
                x = arr[block, s2]
                at = slice(block * quarter, (block + 1) * quarter)
                g = g + dot(x, gate[at, :])
                u = u + dot(x, up[at, :])
            hidden = (jax.nn.silu(g) * u).astype(bf16)
            for half in range(2):
                p_send[s2, half] = dot(hidden, down[:, columns(half * 2 + 1 - jc)]).astype(bf16)
            for half in range(2):
                p_own[s2, half] = dot(hidden, down[:, columns(half * 2 + jc)]).astype(bf16)
            p_copy(s2).start()

        @pl.when((d >= 3) & (d - 3 < n))
        def _():
            p_copy(s3).wait_recv()
            q_send[s3] = (
                p_own[s3, 1 - jx].astype(f32) + p_recv[s3, 1 - jx].astype(f32)
            ).astype(bf16)
            q_copy(s3).start()

        @pl.when((d >= 4) & (d - 4 < n))
        def _():
            q_copy(s4).wait_recv()
            total = (
                p_own[s4, jx].astype(f32) + p_recv[s4, jx].astype(f32) + q_recv[s4].astype(f32)
            ).astype(bf16)

            @pl.when(d == 4)
            def _():
                ret[i] = total

            @pl.when(d > 4)
            def _():
                fin[s4] = total
                back_to(s4).start()

        @pl.when(d <= 4)
        def _():
            conv_piece(d - 1)

        @pl.when(d == 4)
        def _():
            stat_a[...] = stats[...].T[:8, :]
            stat_one().start()

        @pl.when(d == 5)
        def _():
            stat_one().wait()
            stat_c[...] = stat_a[...] + stat_b[...]
            stat_two().start()

        @pl.when(d == 6)
        def _():
            stat_two().wait()
            conv_product()
            c_one().start()

        @pl.when(d == 7)
        def _():
            c_one().wait()
            cq_send[...] = (
                c_own[1 - jx].astype(f32) + c_recv[1 - jx].astype(f32)
            ).astype(bf16)
            c_two().start()

        @pl.when(d == 8)
        def _():
            shared_hidden = (
                jax.nn.silu(dot(norm[...], sg[...])) * dot(norm[...], su[...])
            ).astype(bf16)
            shared[...] = dot(shared_hidden, sd[...])

        return 0

    lax.fori_loop(1, n + 4, step, 0)

    c_two().wait()
    conv_out[...] = (
        c_own[jx].astype(f32) + c_recv[jx].astype(f32) + cq_recv[...].astype(f32)
    ).astype(bf16)

    def combine(e):
        hit = pick(e)
        w = wt_s[pl.ds(e, 1), :]
        high = w.astype(bf16).astype(f32)
        low = w - high
        rows_back = ret[e]
        total = jnp.zeros(shared.shape, f32)
        for part in (high, low):
            m = jnp.where(hit, part, 0.0).astype(bf16)
            total = total + lax.dot_general(
                m, rows_back, (((0,), (0,)), ((), ())), preferred_element_type=f32
            )
        shared[...] += total

    combine(i)

    def gather(d, _):
        e = lax.rem(i + d, n)
        back_from(e).wait_recv()
        combine(e)
        return 0

    lax.fori_loop(1, n, gather, 0)
    moe_out[...] = shared[...].astype(bf16)

    @pl.when(i < n - 1)
    def _():
        halo(i + 1).wait_send()

    def drain(d, _):
        s = lax.rem(i + d, n)
        to_expert(s).wait_send()
        forward(j, s, across, fx_s, fx_r).wait_send()
        forward(j, s, partner, fc_s, fc_r).wait_send()
        forward(block_x, s, partner, f2_s, f2_r).wait_send()
        back_to(s).wait_send()
        return 0

    lax.fori_loop(1, n, drain, 0)

    def drain_all(s, _):
        p_copy(s).wait_send()
        q_copy(s).wait_send()
        return 0

    lax.fori_loop(0, n, drain_all, 0)


def local(
    conv_value, conv_gate, conv_taps, conv_gain, conv_proj, moe_tokens, moe_gain, routes,
    route_weights, expert_gate, expert_up, expert_down, shared_gate, shared_up, shared_down,
):
    n, tp = lax.axis_size("ep"), lax.axis_size("tp")
    assert tp == 4
    rows, width = moe_tokens.shape
    quarter = width // tp
    cap = 3 * rows * routes.shape[1] // (2 * n)
    cap = -(-cap // 16) * 16
    ff = expert_gate.shape[2]
    lead = -(-(conv_taps.shape[0] - 1) // 16) * 16
    vmem = pl.BlockSpec(memory_space=pltpu.VMEM)
    anywhere = pl.BlockSpec(memory_space=pl.ANY)
    V = pltpu.VMEM
    dma = pltpu.SemaphoreType.DMA
    return pl.pallas_call(
        functools.partial(kernel, n, tp, cap),
        out_shape=(
            jax.ShapeDtypeStruct((rows, quarter), bf16),
            jax.ShapeDtypeStruct((rows, quarter), bf16),
        ),
        in_specs=[vmem] * 5 + [anywhere] * 10,
        out_specs=(vmem, vmem),
        scratch_shapes=[
            V((width, ff), bf16), V((width, ff), bf16), V((ff, width), bf16),
            V(shared_gate.shape, bf16), V(shared_up.shape, bf16), V(shared_down.shape, bf16),
            V(conv_proj.shape, bf16),
            V((rows, width), bf16), V((n, rows), jnp.int32), V((n, rows), f32),
            V((n, cap, quarter), bf16), V((tp, n, cap, quarter), bf16),
            V((n, 2, cap, quarter), bf16), V((n, 2, cap, quarter), bf16),
            V((n, 2, cap, quarter), bf16),
            V((n, cap, quarter), bf16), V((n, cap, quarter), bf16),
            V((n, cap, quarter), bf16), V((n, cap, quarter), bf16),
            V((rows, quarter), bf16), V((rows, quarter), bf16), V(conv_taps.shape, bf16),
            V((rows + lead, quarter), f32), V((lead, quarter), bf16), V((lead, quarter), bf16),
            V((rows, quarter), f32), V((rows, 128), f32),
            V((8, rows), f32), V((8, rows), f32), V((8, rows), f32), V((8, rows), f32),
            V((rows, quarter), f32),
            V((2, rows, quarter), bf16), V((2, rows, quarter), bf16), V((2, rows, quarter), bf16),
            V((rows, quarter), bf16), V((rows, quarter), bf16),
            dma((10,)),
        ] + [dma((n,))] * 14 + [dma((8,)), dma((2,))],
        compiler_params=pltpu.CompilerParams(
            collective_id=0, has_side_effects=True, vmem_limit_bytes=60 * 1024 * 1024
        ),
    )(
        moe_tokens, moe_gain[None, :], routes.T, route_weights.T, conv_gain[None, :],
        conv_value, conv_gate, conv_taps,
        expert_gate, expert_up, expert_down, shared_gate, shared_up, shared_down, conv_proj,
    )


def solution(mesh):
    placed = (
        P("ep", "tp"),
        P("ep", "tp"),
        P(None, "tp"),
        P("tp"),
        P("tp", None),
        P("ep", None),
        P(),
        P("ep", None),
        P("ep", None),
        P("ep", None, "tp"),
        P("ep", None, "tp"),
        P("ep", "tp", None),
        P(),
        P(),
        P(None, "tp"),
    )
    return jax.shard_map(
        local, mesh=mesh, in_specs=placed, out_specs=(P("ep", "tp"), P("ep", "tp")), check_vma=False
    )
```
